32 devices in a mesh: sp: 8 (over z, core), tp: 4 (over y, x).
Axes of the slice: x: 2, y: 2, z: 4, core: 2. Of those that a mesh axis runs over, the one named last changes fastest.
Arguments:
- moe_input: bfloat16 [1024, 2048], P('sp', 'tp'), may hold values from -6 to 6
- cotangent: bfloat16 [1024, 2048], P('sp', 'tp'), may hold values from -6 to 6
- routes: int32 [1024, 2], P('sp'), may hold values from 0 to 7, all different within a row; in each aligned block of 128 rows (0 to 127, 128 to 255, ...) at most 64 rows name the same one
- route_weight: float32 [1024, 2], P('sp'), may hold values from 0.1 to 1
- w_gate: bfloat16 [8, 2816, 2048], P('sp', 'tp'), may hold values from -0.125 to 0.125
- w_up: bfloat16 [8, 2816, 2048], P('sp', 'tp'), may hold values from -0.125 to 0.125
- w_down: bfloat16 [8, 2816, 2048], P('sp', 'tp'), may hold values from -0.109375 to 0.109375
- v_value: bfloat16 [1024, 1024], P('sp', 'tp'), may hold values from -6 to 6
- v_gate: bfloat16 [1024, 1024], P('sp', 'tp'), may hold values from -12 to 12
- conv_out: bfloat16 [1024, 1024], P('sp', 'tp'), may hold values from -6 to 6
- row_mean: float32 [1024], P('sp'), may hold values from -3 to 3
- row_rstd: float32 [1024], P('sp'), may hold values from 0.5 to 2
- ln_gain: float32 [1024], P('tp'), may hold values from 0.1 to 1.9
- taps: bfloat16 [31, 1024], P(None, 'tp'), may hold values from -1 to 1
- out_proj: bfloat16 [2048, 1024], P('sp', 'tp'), may hold values from -0.1875 to 0.1875
Outputs:
- gate_grad: bfloat16 [8, 2816, 2048], P('sp', 'tp')
- up_grad: bfloat16 [8, 2816, 2048], P('sp', 'tp')
- down_grad: bfloat16 [8, 2816, 2048], P('sp', 'tp')
- proj_grad: float32 [2048, 1024], P('sp', 'tp')
- stream_grad: bfloat16 [1024, 2048], P('sp', 'tp')
- value_grad: bfloat16 [1024, 1024], P('sp', 'tp')
- gating_grad: bfloat16 [1024, 1024], P('sp', 'tp')
The draws below stay inside these ranges and needn't reach their ends.
Inputs may be any that keep to these rules, and one draw needn't show every extreme that they name: `routes`: in the rows of one device no expert is named more than 64 times.
All inputs are finite; a program needn't handle non-finite values.
Results may differ from the reference program's by a relative error of at most 0.025.
Values may be sent and summed in bfloat16 or wider, within the bound.
A program may use at most 64 MiB of HBM per device.

```python
import math
import jax
import jax.numpy as jnp
import numpy as np
from jax import lax

D = 2048
FF = 2816
CW = 1024
KERNEL = 31
TOK_DEV = 128
TOKENS = 1024
EXPERTS = 8
CAP = 64
N_SP = 8
N_TP = 4


def spiked(values, key, source, target, shards_of, factor):
    def block_of(axis_at):
        return (jnp.arange(values.shape[axis_at]) // (values.shape[axis_at] // shards_of)).reshape((-1,) + (1,) * (values.ndim - 1 - axis_at))

    first = jax.random.permutation(key, shards_of)[block_of(target)]
    other_side = (block_of(target) + shards_of // 2) % shards_of
    return jnp.where((block_of(source) == first) | (block_of(source) == other_side), factor * values, values)


def shard_levels(rng, extent, split, least, top_value):
    loudness = 1.0
    for dim, shards_of in split:
        draws = jax.random.uniform(jax.random.fold_in(jax.random.fold_in(rng, 6), dim), (shards_of,), jnp.float32, least / len(split), top_value / len(split))
        loudness = loudness * jnp.repeat(jnp.exp(draws), extent[dim] // shards_of).reshape((-1,) + (1,) * (len(extent) - 1 - dim))
    return loudness


def routed_block(rng, own, number, rows, number_of, top, bound, lean):
    sequence = jax.random.permutation(rng, number_of)
    crowded, usual = portions_of(number_of, rows * top, bound, lean, True), portions_of(number_of, rows * top, bound, lean, False)
    places = jnp.arange(number_of)

    def named(sizes, offset_by):
        used = int((sizes > 0).sum())
        fixed = max(1, used // 4)
        passed = fixed + (places - fixed + offset_by * (used - fixed)) % max(1, number_of - fixed)
        return jnp.zeros((number_of,), jnp.int32).at[sequence[jnp.where(places < fixed, places, passed)]].set(jnp.asarray(sizes, jnp.int32))

    sizes = jnp.where(number % 4 == 0, named(crowded, number // 4), named(usual, number - number // 4 - 1))
    mixed = jax.random.permutation(jax.random.fold_in(own, 3), number_of)
    source_of, receiver = mixed[0:number_of // 2 * 2:2], mixed[1:number_of // 2 * 2:2]
    slack = jnp.minimum(sizes[source_of] - 1, bound - sizes[receiver]) // 2
    slack = jnp.where((source_of == sequence[0]) | (receiver == sequence[0]) | (sizes[receiver] == 0), 0, jnp.maximum(slack, 0))
    passed = jax.random.randint(jax.random.fold_in(own, 4), (number_of // 2,), 0, 1 << 20) % (slack + 1)
    sizes = sizes.at[source_of].add(-passed).at[receiver].add(passed)
    members = jnp.searchsorted(jnp.cumsum(sizes), jnp.arange(rows * top), side="right").astype(jnp.int32)
    table = members.reshape(top, rows).T
    table = table[jax.random.permutation(jax.random.fold_in(own, 1), rows)]
    offset_by = jax.random.randint(jax.random.fold_in(own, 2), (rows, 1), 0, top)
    return jnp.take_along_axis(table, (jnp.arange(top)[None, :] + offset_by) % top, axis=1)


def portions_of(number_of, total, reach, lean, full):
    portions = [(1 << 20) // math.isqrt(standing ** lean) + 1 for standing in range(1, number_of + 1)]
    largest = reach if full else min(reach, max(-(-total // number_of), total * portions[0] // sum(portions)))
    least = 1 if total - largest >= number_of - 1 else 0
    holding, rest = [largest] + [least] * (number_of - 1), total - largest - least * (number_of - 1)
    while rest > 0:
        movable = [i for i in range(1, number_of) if holding[i] < largest] or [i for i in range(1, number_of) if holding[i] < reach]
        pool, budget = sum([portions[i] for i in movable]), rest
        for i in movable:
            addition = min(reach - holding[i], max(1, budget * portions[i] // pool), rest)
            holding[i] = holding[i] + addition
            rest = rest - addition
    return np.array(holding)


def scatter_about(rng, shape, deviation, reach, shards=(), kind=jnp.bfloat16):
    array = jax.random.normal(rng, shape, jnp.float32) * deviation
    if len(shards) > 0:
        array = shard_levels(rng, shape, shards, -0.22, 0.18) * array
    return jnp.clip(array, min=-reach, max=reach).astype(kind)


def heavy_noise(stream_key, dims, deviation, most, shards, heavy, kind=jnp.bfloat16):
    values = deviation * jax.random.normal(stream_key, dims, jnp.float32)
    if shards:
        values = values * shard_levels(stream_key, dims, shards, -0.22, 0.18)
    return jnp.clip(spiked(values, jax.random.fold_in(stream_key, 3), *heavy), -most, most).astype(kind)


def setup_inputs(seed: int = 0) -> dict:
    key_list = jax.random.split(jax.random.key(seed), 16)
    moe_input = scatter_about(key_list[0], (TOKENS, D), 1.0, 6.0, ((0, 8), (1, 4)))
    cotangent = heavy_noise(key_list[1], (TOKENS, D), 1.0, 6.0, ((0, 8), (1, 4)), (0, 1, 8, 2.0))
    routes_keys = jax.random.split(jax.random.fold_in(key_list[2], 1), TOKENS // TOK_DEV)
    routes_turns = jax.random.permutation(jax.random.fold_in(key_list[2], 3), TOKENS // TOK_DEV)
    routes = jax.vmap(lambda own, number: routed_block(jax.random.fold_in(key_list[2], 2), own, number, TOK_DEV, EXPERTS, 2, CAP, 2))(routes_keys, routes_turns).reshape((TOKENS, 2))
    route_weight = jnp.clip(0.1 + 0.9 * jax.random.uniform(key_list[3], (TOKENS, 2), jnp.float32) ** shard_levels(key_list[3], (TOKENS, 2), ((0, 8),), -0.2, 0.2), 0.1, 1.0)
    w_gate = scatter_about(key_list[4], (EXPERTS, FF, D), D ** -0.5, 0.125, ((0, 8), (1, 4)))
    w_up = scatter_about(key_list[5], (EXPERTS, FF, D), D ** -0.5, 0.125, ((0, 8), (1, 4)))
    w_down = scatter_about(key_list[6], (EXPERTS, FF, D), FF ** -0.5, 0.109375, ((0, 8), (1, 4)))
    v_value = scatter_about(key_list[7], (TOKENS, CW), 1.0, 6.0, ((0, 8), (1, 4)))
    v_gate = scatter_about(key_list[8], (TOKENS, CW), 2.0, 12.0, ((0, 8), (1, 4)))
    conv_out = scatter_about(key_list[9], (TOKENS, CW), 1.0, 6.0, ((0, 8), (1, 4)))
    row_mean = scatter_about(key_list[10], (TOKENS,), 0.5, 3.0, ((0, 8),), jnp.float32)
    row_rstd = jnp.clip(jnp.exp(math.log(2.0) - 1.3862944 * jax.random.uniform(key_list[11], (TOKENS,), jnp.float32) ** shard_levels(key_list[11], (TOKENS,), ((0, 8),), -0.2, 0.2)), 0.5, 2.0)
    ln_gain = jnp.clip(1.0 + 0.18 * jax.random.normal(key_list[12], (CW,), jnp.float32), 0.1, 1.9)
    taps = scatter_about(key_list[13], (KERNEL, CW), KERNEL ** -0.5, 1.0, ((1, 4),))
    out_proj = scatter_about(key_list[14], (D, CW), CW ** -0.5, 0.1875, ((0, 8), (1, 4)))
    return {"moe_input": moe_input, "cotangent": cotangent, "routes": routes, "route_weight": route_weight, "w_gate": w_gate, "w_up": w_up, "w_down": w_down, "v_value": v_value, "v_gate": v_gate, "conv_out": conv_out, "row_mean": row_mean, "row_rstd": row_rstd, "ln_gain": ln_gain, "taps": taps, "out_proj": out_proj}


def slot_numbers(block_routes):
    member = (block_routes[:, None] == jnp.arange(N_SP, dtype=jnp.int32)[None, :]).astype(jnp.int32)
    earlier = jnp.cumsum(member, axis=0) - member
    return jnp.sum(earlier * member, axis=1).astype(jnp.int32)


def expert_pass(operands):
    rows, cotan, gate_w, up_w, down_w = operands
    total = rows.shape[0]
    gate_pre = jnp.dot(rows, gate_w.T, preferred_element_type=jnp.float32)
    up_pre = jnp.dot(rows, up_w.T, preferred_element_type=jnp.float32)
    gate_sig = jax.nn.sigmoid(gate_pre)
    gate_act = gate_pre * gate_sig
    hidden = (gate_act * up_pre).astype(jnp.bfloat16)
    down_g = jnp.dot(hidden.T, cotan, preferred_element_type=jnp.float32).astype(jnp.bfloat16)
    hidden_grad = jnp.dot(cotan, down_w.T, preferred_element_type=jnp.float32)
    gate_delta = (hidden_grad * up_pre * gate_sig * (1.0 + gate_pre * (1.0 - gate_sig))).astype(jnp.bfloat16)
    up_delta = (hidden_grad * gate_act).astype(jnp.bfloat16)
    gate_g = jnp.dot(gate_delta.T, rows, preferred_element_type=jnp.float32).astype(jnp.bfloat16)
    up_g = jnp.dot(up_delta.T, rows, preferred_element_type=jnp.float32).astype(jnp.bfloat16)
    per_block = FF // N_TP
    gate_three = gate_delta.astype(jnp.float32).reshape(total, N_TP, per_block)
    up_three = up_delta.astype(jnp.float32).reshape(total, N_TP, per_block)
    gate_wt = gate_w.astype(jnp.float32).reshape(N_TP, per_block, D)
    up_wt = up_w.astype(jnp.float32).reshape(N_TP, per_block, D)
    partial_value = jnp.einsum('rnf,nfd->nrd', gate_three, gate_wt) + jnp.einsum('rnf,nfd->nrd', up_three, up_wt)
    rounded = lax.optimization_barrier(partial_value.astype(jnp.bfloat16))
    row_g = jnp.sum(rounded.astype(jnp.float32), axis=0).astype(jnp.bfloat16)
    return gate_g, up_g, down_g, row_g


def reference(moe_input, cotangent, routes, route_weight, w_gate, w_up, w_down, v_value, v_gate,
              conv_out, row_mean, row_rstd, ln_gain, taps, out_proj):
    buffer_len = N_SP * CAP
    block_routes = routes.reshape(N_SP, 2 * TOK_DEV).astype(jnp.int32)
    slot_index = jax.vmap(slot_numbers)(block_routes)
    source = jnp.arange(N_SP, dtype=jnp.int32)[:, None]
    buffer_row = (block_routes * buffer_len + source * CAP + slot_index).reshape(-1).astype(jnp.int32)
    token_index = (jnp.arange(2 * TOKENS, dtype=jnp.int32) // 2).astype(jnp.int32)
    picked = moe_input[token_index]
    weighted = (route_weight.reshape(-1)[:, None] * cotangent[token_index].astype(jnp.float32)).astype(jnp.bfloat16)
    rows_all = jnp.zeros((EXPERTS * buffer_len, D), jnp.bfloat16).at[buffer_row].set(picked)
    cotan_all = jnp.zeros((EXPERTS * buffer_len, D), jnp.bfloat16).at[buffer_row].set(weighted)
    rows_all = rows_all.reshape(EXPERTS, buffer_len, D)
    cotan_all = cotan_all.reshape(EXPERTS, buffer_len, D)
    gate_g, up_g, down_g, row_g = lax.map(expert_pass, (rows_all, cotan_all, w_gate, w_up, w_down))
    returned = row_g.reshape(EXPERTS * buffer_len, D)[buffer_row].astype(jnp.float32)
    returned = returned.reshape(TOKENS, 2, D)
    stream = cotangent.astype(jnp.float32) + (returned[:, 0] + returned[:, 1])
    stream = stream.astype(jnp.bfloat16)
    normed = (conv_out.astype(jnp.float32) - row_mean[:, None]) * row_rstd[:, None]
    scaled_norm = normed * ln_gain[None, :]
    norm_sig = jax.nn.sigmoid(scaled_norm)
    mixed = (scaled_norm * norm_sig).astype(jnp.bfloat16)
    mixed_grad = jnp.dot(stream, out_proj, preferred_element_type=jnp.float32)
    proj_g = jnp.dot(stream.T, mixed, preferred_element_type=jnp.float32)
    norm_grad = mixed_grad * norm_sig * (1.0 + scaled_norm * (1.0 - norm_sig)) * ln_gain[None, :]
    first_mean = jnp.mean(norm_grad, axis=1, keepdims=True)
    second_mean = jnp.mean(norm_grad * normed, axis=1, keepdims=True)
    conv_grad = row_rstd[:, None] * (norm_grad - first_mean - normed * second_mean)
    extended = jnp.concatenate([conv_grad, jnp.zeros((KERNEL - 1, CW), jnp.float32)], axis=0)
    tap_values = taps.astype(jnp.float32)
    unit_grad = jnp.zeros((TOKENS, CW), jnp.float32)
    for offset in range(KERNEL):
        lead = KERNEL - 1 - offset
        unit_grad = unit_grad + tap_values[offset][None, :] * extended[lead:lead + TOKENS]
    gate_sig = jax.nn.sigmoid(v_gate.astype(jnp.float32))
    value_g = (unit_grad * gate_sig).astype(jnp.bfloat16)
    gating_g = (unit_grad * v_value.astype(jnp.float32) * gate_sig * (1.0 - gate_sig)).astype(jnp.bfloat16)
    return (gate_g, up_g, down_g, proj_g, stream, value_g, gating_g)
```

```python
import functools

import jax
import jax.numpy as jnp
from jax import lax
from jax.experimental import pallas as pl
from jax.experimental.pallas import tpu as pltpu
from jax.sharding import PartitionSpec as P


def passed_along(value, axis, steps):
    count = lax.axis_size(axis)
    leading, last = (max(0, -steps), min(count, count - steps))
    return lax.ppermute(value, axis, [(source, source + steps) for source in range(leading, last)])


def route_targets(routes, experts, capacity):
    flat_routes = routes.reshape(-1)
    member = (flat_routes[:, None] == jnp.arange(experts, dtype=jnp.int32)[None, :]).astype(
        jnp.int32
    )
    earlier = jnp.cumsum(member, axis=0) - member
    slot_index = jnp.sum(earlier * member, axis=1)
    return flat_routes * capacity + slot_index


def contract_rows(left, right):
    return lax.dot_general(
        left, right, (((0,), (0,)), ((), ())), preferred_element_type=jnp.float32
    )


def contract_cols(left, right):
    return lax.dot_general(
        left, right, (((1,), (1,)), ((), ())), preferred_element_type=jnp.float32
    )


def plain_shards(
    moe_input,
    cotangent,
    routes,
    route_weight,
    w_gate,
    w_up,
    w_down,
    v_value,
    v_gate,
    conv_out,
    row_mean,
    row_rstd,
    ln_gain,
    taps,
    out_proj,
):
    experts = lax.axis_size("sp")
    tokens = routes.shape[0]
    capacity = 4 * tokens // experts
    total = experts * capacity
    buffer_row = route_targets(routes, experts, capacity)
    token_index = jnp.arange(2 * tokens, dtype=jnp.int32) // 2
    weights = route_weight.reshape(-1)
    width = moe_input.shape[1]
    picked = moe_input[token_index]
    weighted = (weights[:, None] * cotangent[token_index].astype(jnp.float32)).astype(jnp.bfloat16)
    rows_buf = jnp.zeros((total, width), jnp.bfloat16).at[buffer_row].set(picked)
    cotan_buf = jnp.zeros((total, width), jnp.bfloat16).at[buffer_row].set(weighted)
    rows_buf, cotan_buf = (
        rows_buf.reshape(experts, capacity, width),
        cotan_buf.reshape(experts, capacity, width),
    )
    part_rows, part_cotan = (
        lax.all_to_all(rows_buf, "sp", split_axis=0, concat_axis=0, tiled=True),
        lax.all_to_all(cotan_buf, "sp", split_axis=0, concat_axis=0, tiled=True),
    )
    arrived_rows, arrived_cotan = (
        lax.all_gather(part_rows, "tp", axis=2, tiled=True),
        lax.all_gather(part_cotan, "tp", axis=2, tiled=True),
    )
    width = arrived_rows.shape[2]
    expert_in = arrived_rows.reshape(total, width)
    expert_cot = arrived_cotan.reshape(total, width)
    gate_w = w_gate[0]
    up_w = w_up[0]
    down_w = w_down[0]
    gate_pre = contract_cols(expert_in, gate_w)
    up_pre = contract_cols(expert_in, up_w)
    gate_sig = jax.nn.sigmoid(gate_pre)
    gate_act = gate_pre * gate_sig
    hidden = (gate_act * up_pre).astype(jnp.bfloat16)
    down_g = contract_rows(hidden, expert_cot).astype(jnp.bfloat16)
    hidden_grad = contract_cols(expert_cot, down_w)
    gate_delta = (hidden_grad * up_pre * gate_sig * (1.0 + gate_pre * (1.0 - gate_sig))).astype(
        jnp.bfloat16
    )
    up_delta = (hidden_grad * gate_act).astype(jnp.bfloat16)
    gate_g = contract_rows(gate_delta, expert_in).astype(jnp.bfloat16)
    up_g = contract_rows(up_delta, expert_in).astype(jnp.bfloat16)
    partial_value = jnp.dot(gate_delta, gate_w, preferred_element_type=jnp.float32) + jnp.dot(
        up_delta, up_w, preferred_element_type=jnp.float32
    )
    row_share = lax.psum_scatter(
        partial_value.astype(jnp.bfloat16), "tp", scatter_dimension=1, tiled=True
    )
    slice_width = row_share.shape[1]
    returned = lax.all_to_all(
        row_share.reshape(experts, capacity, slice_width),
        "sp",
        split_axis=0,
        concat_axis=0,
        tiled=True,
    )
    mine = (
        returned.reshape(total, slice_width)[buffer_row]
        .astype(jnp.float32)
        .reshape(tokens, 2, slice_width)
    )
    stream = (cotangent.astype(jnp.float32) + (mine[:, 0] + mine[:, 1])).astype(jnp.bfloat16)
    full_stream = lax.all_gather(stream, "tp", axis=1, tiled=True)
    normed = (conv_out.astype(jnp.float32) - row_mean[:, None]) * row_rstd[:, None]
    scaled_norm = normed * ln_gain[None, :]
    norm_sig = jax.nn.sigmoid(scaled_norm)
    mixed = (scaled_norm * norm_sig).astype(jnp.bfloat16)
    columns = full_stream
    mixed_grad = jnp.dot(
        columns,
        lax.all_gather(out_proj, "sp", axis=0, tiled=True),
        preferred_element_type=jnp.float32,
    )
    columns = full_stream
    proj_g = lax.psum_scatter(
        contract_rows(columns, mixed).astype(jnp.bfloat16), "sp", scatter_dimension=0, tiled=True
    ).astype(jnp.float32)
    channels = out_proj.shape[1] * lax.axis_size("tp")
    norm_grad = mixed_grad * norm_sig * (1.0 + scaled_norm * (1.0 - norm_sig)) * ln_gain[None, :]
    first_sum, second_sum = lax.psum(
        (jnp.sum(norm_grad, axis=1), jnp.sum(norm_grad * normed, axis=1)), "tp"
    )
    first_mean = first_sum[:, None] / channels
    second_mean = second_sum[:, None] / channels
    conv_grad = row_rstd[:, None] * (norm_grad - first_mean - normed * second_mean)
    kernel = taps.shape[0]
    following = passed_along(conv_grad[: kernel - 1], "sp", -1)
    extended = jnp.concatenate([conv_grad, following], axis=0)
    tap_values = taps.astype(jnp.float32)
    unit_grad = jnp.zeros_like(conv_grad)
    for offset in range(kernel):
        lead = kernel - 1 - offset
        unit_grad = unit_grad + tap_values[offset][None, :] * extended[lead : lead + tokens]
    value_sig = jax.nn.sigmoid(v_gate.astype(jnp.float32))
    value_g = (unit_grad * value_sig).astype(jnp.bfloat16)
    gating_g = (unit_grad * v_value.astype(jnp.float32) * value_sig * (1.0 - value_sig)).astype(
        jnp.bfloat16
    )
    return (gate_g[None], up_g[None], down_g[None], proj_g, stream, value_g, gating_g)


VMEM = pl.BlockSpec(memory_space=pltpu.VMEM)


def remote(src, dst, send_sem, recv_sem, sp, tp):
    return pltpu.make_async_remote_copy(
        src_ref=src,
        dst_ref=dst,
        send_sem=send_sem,
        recv_sem=recv_sem,
        device_id={"sp": sp, "tp": tp},
        device_id_type=pl.DeviceIdType.MESH,
    )


def greet(peers):
    barrier = pltpu.get_barrier_semaphore()
    for sp, tp in peers:
        pl.semaphore_signal(
            barrier, inc=1, device_id={"sp": sp, "tp": tp}, device_id_type=pl.DeviceIdType.MESH
        )
    pl.semaphore_wait(barrier, len(peers))


def rows_of(ref, index, count):
    return ref.at[pl.ds(pl.multiple_of(index * count, count), count)]


class ChipGather:
    def __init__(self, own, everyone, sems, me, tp, count):
        self.own, self.everyone, self.me, self.tp, self.count = own, everyone, me, tp, count
        self.send, self.recv, self.relay, self.local = sems
        self.partner = me + 1 - 2 * (me % 2)
        self.ahead = [(me + 2 * e) % count for e in range(1, count // 2)]
        self.behind = [(me + count - 2 * e) % count for e in range(1, count // 2)]

    def block(self, index):
        return rows_of(self.everyone, index, self.own.shape[0])

    def first(self, target):
        return remote(
            self.own,
            self.block(self.me),
            self.send.at[target],
            self.recv.at[self.me],
            target,
            self.tp,
        )

    def onward(self, origin):
        return remote(
            self.block(origin),
            self.block(origin),
            self.relay.at[origin],
            self.recv.at[origin],
            self.partner,
            self.tp,
        )

    def start(self):
        pltpu.make_async_copy(self.own, self.block(self.me), self.local).start()
        for target in self.ahead + [self.partner]:
            self.first(target).start()

    def pass_on(self):
        for origin in self.behind:
            self.onward(origin).wait_recv()
            self.onward(origin).start()

    def finish(self):
        pltpu.make_async_copy(self.own, self.block(self.me), self.local).wait()
        for step in range(self.count // 2):
            origin = (self.partner + 2 * step) % self.count
            self.onward(origin).wait_recv()
        for target in self.ahead + [self.partner]:
            self.first(target).wait_send()
        for origin in self.behind:
            self.onward(origin).wait_send()


def gather_sems(count):
    return [
        pltpu.SemaphoreType.DMA((count,)),
        pltpu.SemaphoreType.DMA((count,)),
        pltpu.SemaphoreType.DMA((count,)),
        pltpu.SemaphoreType.DMA,
    ]


def dispatch_kernel(
    count, rows, cot, mixed, rows_out, cot_out, mixed_out, send, recv, local, *mixed_sems
):
    me, tp = lax.axis_index("sp"), lax.axis_index("tp")
    capacity, width = rows.shape[1:]
    across, down, corner = tp + 1 - 2 * (tp % 2), (tp + 2) % 4, 3 - tp
    others = [(me + d) % count for d in range(1, count)]
    greet([(other, tp) for other in others] + [(me, across), (me, down)])
    arrays = ((rows, rows_out), (cot, cot_out))

    def block(a, source, owner):
        return arrays[a][1].at[
            pl.ds(pl.multiple_of(source * capacity, capacity), capacity),
            pl.ds(pl.multiple_of(owner * width, 128), width),
        ]

    def own_copy(a):
        return pltpu.make_async_copy(arrays[a][0].at[me], block(a, me, tp), local.at[a])

    def out_copy(a, target):
        return remote(
            arrays[a][0].at[target],
            block(a, me, tp),
            send.at[a, target, 0],
            recv.at[a, me, tp],
            target,
            tp,
        )

    def side_copy(a, source, owner, target, lane):
        spot = block(a, source, owner)
        return remote(spot, spot, send.at[a, source, lane], recv.at[a, source, owner], me, target)

    for a in range(2):
        own_copy(a).start()
    for target in others:
        for a in range(2):
            out_copy(a, target).start()
    gather = ChipGather(mixed, mixed_out, mixed_sems, me, tp, count)
    gather.start()

    def relay_of(step):
        return (across, down) if step % 2 == 0 else (down, across)

    def relay(step):
        source = (me + count - step) % count
        owner, target = relay_of(step)
        for a in range(2):
            side_copy(a, source, owner, target, 3).wait_recv()
            side_copy(a, source, owner, target, 3).start()

    for step in range(count):
        source = (me + count - step) % count
        for a in range(2):
            if step == 0:
                own_copy(a).wait()
            else:
                side_copy(a, source, tp, across, 1).wait_recv()
            side_copy(a, source, tp, across, 1).start()
            side_copy(a, source, tp, down, 2).start()
        if step >= 1:
            relay(step - 1)
    relay(count - 1)
    gather.pass_on()
    for step in range(count):
        source = (me + count - step) % count
        owner, target = relay_of(step)
        for a in range(2):
            side_copy(a, source, target, across, 1).wait_recv()
            side_copy(a, source, corner, across, 1).wait_recv()
            side_copy(a, source, tp, across, 1).wait_send()
            side_copy(a, source, tp, down, 2).wait_send()
            side_copy(a, source, owner, target, 3).wait_send()
    for target in others:
        for a in range(2):
            out_copy(a, target).wait_send()
    gather.finish()


def dispatch(rows, cot, mixed, count):
    capacity, width = rows.shape[1:]
    full = jax.ShapeDtypeStruct((count * capacity, width * lax.axis_size("tp")), jnp.bfloat16)
    return pl.pallas_call(
        functools.partial(dispatch_kernel, count),
        out_shape=(
            full,
            full,
            jax.ShapeDtypeStruct((count * mixed.shape[0], mixed.shape[1]), mixed.dtype),
        ),
        in_specs=[VMEM] * 3,
        out_specs=(VMEM,) * 3,
        scratch_shapes=[
            pltpu.SemaphoreType.DMA((2, count, 4)),
            pltpu.SemaphoreType.DMA((2, count, 4)),
            pltpu.SemaphoreType.DMA((2,)),
        ]
        + gather_sems(count),
        compiler_params=pltpu.CompilerParams(
            collective_id=0, has_side_effects=True, vmem_limit_bytes=40 << 20
        ),
        name="dispatch",
    )(rows, cot, mixed)


def combine_kernel(
    count,
    partial_ref,
    cot,
    pick,
    proj,
    stream,
    proj_out,
    landed,
    reduced,
    back,
    send,
    recv,
    back_send,
    back_recv,
    wide_send,
    wide_recv,
    *proj_sems,
):
    me, tp = lax.axis_index("sp"), lax.axis_index("tp")
    capacity, width = reduced.shape[1:]
    group = (tp + 1 - 2 * (tp % 2), (tp + 2) % 4, 3 - tp)
    others = [(me + d) % count for d in range(1, count)]
    greet([(other, tp) for other in others] + [(me, other) for other in group])

    def share(source, owner):
        return partial_ref.at[
            pl.ds(pl.multiple_of(source * capacity, capacity), capacity),
            pl.ds(pl.multiple_of(owner * width, 128), width),
        ]

    def share_copy(source, q):
        return remote(
            share(source, group[q]),
            landed.at[q, source],
            send.at[source, q],
            recv.at[source, q],
            me,
            group[q],
        )

    def back_copy(target):
        return remote(
            reduced.at[target],
            rows_of(back, me, capacity),
            back_send.at[target],
            back_recv.at[me],
            target,
            tp,
        )

    order = others + [me]
    for source in order:
        for q in range(3):
            share_copy(source, q).start()
    gather = ChipGather(proj, proj_out, proj_sems, me, tp, count)
    gather.start()
    for step, source in enumerate(order):
        total = share(source, tp)[...].astype(jnp.float32)
        for q in range(3):
            share_copy(source, q).wait_recv()
            total = total + landed[q, source].astype(jnp.float32)
        total = total.astype(jnp.bfloat16)
        if step < count - 1:
            reduced[source] = total
            back_copy(source).start()
        else:
            back[pl.ds(pl.multiple_of(me * capacity, capacity), capacity), :] = total
    gather.pass_on()
    for other in others:
        remote(
            reduced.at[other],
            rows_of(back, other, capacity),
            back_send.at[other],
            back_recv.at[other],
            other,
            tp,
        ).wait_recv()
    mine = jnp.dot(pick[...], back[...], preferred_element_type=jnp.float32)
    columns = pl.ds(pl.multiple_of(tp * width, 128), width)
    stream[:, columns] = (cot[...].astype(jnp.float32) + mine).astype(jnp.bfloat16)

    def wide_copy(q):
        spot = stream.at[:, columns]
        return remote(spot, spot, wide_send.at[q], wide_recv.at[q], me, group[q])

    for q in range(3):
        wide_copy(q).start()
    for q in range(3):
        wide_copy(q).wait()
    for source in order:
        for q in range(3):
            share_copy(source, q).wait_send()
    for other in others:
        back_copy(other).wait_send()
    gather.finish()


def combine(partial_value, cot, pick, proj, count):
    tokens, width = cot.shape
    capacity = partial_value.shape[0] // count
    return pl.pallas_call(
        functools.partial(combine_kernel, count),
        out_shape=(
            jax.ShapeDtypeStruct((tokens, partial_value.shape[1]), jnp.bfloat16),
            jax.ShapeDtypeStruct((count * proj.shape[0], proj.shape[1]), jnp.bfloat16),
        ),
        in_specs=[VMEM] * 4,
        out_specs=(VMEM,) * 2,
        scratch_shapes=[
            pltpu.VMEM((3, count, capacity, width), jnp.bfloat16),
            pltpu.VMEM((count, capacity, width), jnp.bfloat16),
            pltpu.VMEM((count * capacity, width), jnp.bfloat16),
            pltpu.SemaphoreType.DMA((count, 3)),
            pltpu.SemaphoreType.DMA((count, 3)),
            pltpu.SemaphoreType.DMA((count,)),
            pltpu.SemaphoreType.DMA((count,)),
            pltpu.SemaphoreType.DMA((3,)),
            pltpu.SemaphoreType.DMA((3,)),
        ]
        + gather_sems(count),
        compiler_params=pltpu.CompilerParams(
            collective_id=1, has_side_effects=True, vmem_limit_bytes=40 << 20
        ),
        name="combine",
    )(partial_value, cot, pick, proj)


def module_kernel(
    count,
    stream,
    proj,
    mixed,
    conv_out,
    row_mean,
    row_rstd,
    gain,
    taps,
    v_value,
    v_gate,
    proj_grad,
    value_grad,
    gating_grad,
    columns,
    sums,
    arrived,
    extended,
    send,
    recv,
    local,
    sum_send,
    sum_recv,
    edge_send,
    edge_recv,
):
    me, tp = lax.axis_index("sp"), lax.axis_index("tp")
    tokens, channels = conv_out.shape
    depth = stream.shape[1] // count
    halo = extended.shape[0] - tokens
    group = (tp + 1 - 2 * (tp % 2), (tp + 2) % 4, 3 - tp)
    others = [(me + d) % count for d in range(1, count)]
    greet([(other, tp) for other in others] + [(me, other) for other in group])

    def strip(index):
        return stream.at[:, pl.ds(pl.multiple_of(index * depth, 128), depth)]

    def strip_copy(target):
        return remote(
            strip(target),
            rows_of(columns, me, tokens),
            send.at[target],
            recv.at[me],
            target,
            tp,
        )

    own = pltpu.make_async_copy(strip(me), rows_of(columns, me, tokens), local)
    own.start()
    for other in others:
        strip_copy(other).start()
    mixed_grad = jnp.dot(stream[...], proj[...], preferred_element_type=jnp.float32)
    normed = (conv_out[...].astype(jnp.float32) - row_mean[...]) * row_rstd[...]
    scaled = normed * gain[...]
    sig = jax.nn.sigmoid(scaled)
    norm_grad = mixed_grad * sig * (1.0 + scaled * (1.0 - sig)) * gain[...]
    first = jnp.sum(norm_grad, axis=1, keepdims=True)
    second = jnp.sum(norm_grad * normed, axis=1, keepdims=True)
    lanes = lax.broadcasted_iota(jnp.int32, (tokens, 128), 1)
    pair = jnp.where(lanes % 2 == 0, first, second)
    sums[...] = pair.T[:8]

    def sum_copy(q):
        return remote(sums, arrived.at[q], sum_send.at[q], sum_recv.at[q], me, group[q])

    for q in range(3):
        sum_copy(q).start()
    value_sig = jax.nn.sigmoid(v_gate[...].astype(jnp.float32))
    gating_scale = v_value[...].astype(jnp.float32) * value_sig * (1.0 - value_sig)
    for q in range(3):
        sum_copy(q).wait()
    total = sums[...] + arrived[0] + arrived[1] + arrived[2]
    total = total * (1.0 / (channels * 4))
    means = jnp.concatenate([total] * 16, axis=0).T
    conv_grad = row_rstd[...] * (norm_grad - means[:, 0:1] - normed * means[:, 1:2])
    extended[:tokens] = conv_grad
    edge = remote(
        extended.at[pl.ds(0, halo)],
        extended.at[pl.ds(tokens, halo)],
        edge_send,
        edge_recv,
        (me + count - 1) % count,
        tp,
    )

    @pl.when(me > 0)
    def _():
        edge.start()

    @pl.when(me == count - 1)
    def _():
        extended[tokens:] = jnp.zeros((halo, channels), jnp.float32)

    @pl.when(me < count - 1)
    def _():
        edge.wait_recv()

    kernel = taps.shape[0]
    unit_grad = jnp.zeros((tokens, channels), jnp.float32)
    for offset in range(kernel):
        lead = kernel - 1 - offset
        tap = taps[offset : offset + 1, :].astype(jnp.float32)
        unit_grad = unit_grad + tap * extended[lead : lead + tokens, :]
    value_grad[...] = (unit_grad * value_sig).astype(jnp.bfloat16)
    gating_grad[...] = (unit_grad * gating_scale).astype(jnp.bfloat16)
    own.wait()
    for other in others:
        remote(
            strip(other),
            rows_of(columns, other, tokens),
            send.at[other],
            recv.at[other],
            other,
            tp,
        ).wait_recv()
    proj_grad[...] = contract_rows(columns[...], mixed[...])
    for other in others:
        strip_copy(other).wait_send()

    @pl.when(me > 0)
    def _():
        edge.wait_send()


def module(stream, proj, mixed, conv_out, row_mean, row_rstd, gain, taps, v_value, v_gate, count):
    tokens, channels = conv_out.shape
    depth = stream.shape[1] // count
    halo = -(-(taps.shape[0] - 1) // 8) * 8
    return pl.pallas_call(
        functools.partial(module_kernel, count),
        out_shape=(
            jax.ShapeDtypeStruct((depth, channels), jnp.float32),
            jax.ShapeDtypeStruct((tokens, channels), jnp.bfloat16),
            jax.ShapeDtypeStruct((tokens, channels), jnp.bfloat16),
        ),
        in_specs=[VMEM] * 10,
        out_specs=(VMEM,) * 3,
        scratch_shapes=[
            pltpu.VMEM((count * tokens, depth), jnp.bfloat16),
            pltpu.VMEM((8, tokens), jnp.float32),
            pltpu.VMEM((3, 8, tokens), jnp.float32),
            pltpu.VMEM((tokens + halo, channels), jnp.float32),
            pltpu.SemaphoreType.DMA((count,)),
            pltpu.SemaphoreType.DMA((count,)),
            pltpu.SemaphoreType.DMA,
            pltpu.SemaphoreType.DMA((3,)),
            pltpu.SemaphoreType.DMA((3,)),
            pltpu.SemaphoreType.DMA,
            pltpu.SemaphoreType.DMA,
        ],
        compiler_params=pltpu.CompilerParams(
            collective_id=2, has_side_effects=True, vmem_limit_bytes=40 << 20
        ),
        name="module",
    )(stream, proj, mixed, conv_out, row_mean, row_rstd, gain, taps, v_value, v_gate)


def kernel_shards(
    moe_input,
    cotangent,
    routes,
    route_weight,
    w_gate,
    w_up,
    w_down,
    v_value,
    v_gate,
    conv_out,
    row_mean,
    row_rstd,
    ln_gain,
    taps,
    out_proj,
):
    experts = lax.axis_size("sp")
    tokens, width = moe_input.shape
    capacity = 4 * tokens // experts
    total = experts * capacity
    flat_routes = routes.reshape(-1)
    member = (flat_routes[:, None] == jnp.arange(experts, dtype=jnp.int32)[None, :]).astype(
        jnp.bfloat16
    )
    index = jnp.arange(2 * tokens, dtype=jnp.int32)
    before = (index[None, :] < index[:, None]).astype(jnp.bfloat16)
    earlier = jnp.dot(before, member, preferred_element_type=jnp.float32)
    slot_index = jnp.sum(earlier * member.astype(jnp.float32), axis=1).astype(jnp.int32)
    buffer_row = (flat_routes * capacity + slot_index).reshape(tokens, 2)
    places = jnp.arange(total, dtype=jnp.int32)
    place0 = (buffer_row[:, 0][:, None] == places[None, :]).astype(jnp.bfloat16)
    place1 = (buffer_row[:, 1][:, None] == places[None, :]).astype(jnp.bfloat16)
    pick = place0 + place1
    cot32 = cotangent.astype(jnp.float32)
    weighted = jnp.concatenate(
        [
            (route_weight[:, 0:1] * cot32).astype(jnp.bfloat16),
            (route_weight[:, 1:2] * cot32).astype(jnp.bfloat16),
        ],
        axis=0,
    )
    rows_buf = contract_rows(pick, moe_input).astype(jnp.bfloat16)
    cot_buf = contract_rows(jnp.concatenate([place0, place1], axis=0), weighted).astype(
        jnp.bfloat16
    )
    normed = (conv_out.astype(jnp.float32) - row_mean[:, None]) * row_rstd[:, None]
    scaled_norm = normed * ln_gain[None, :]
    mixed = (scaled_norm * jax.nn.sigmoid(scaled_norm)).astype(jnp.bfloat16)
    expert_in, expert_cot, mixed_all = dispatch(
        rows_buf.reshape(experts, capacity, width),
        cot_buf.reshape(experts, capacity, width),
        mixed,
        experts,
    )
    gate_w = w_gate[0]
    up_w = w_up[0]
    down_w = w_down[0]
    gate_pre = contract_cols(expert_in, gate_w)
    up_pre = contract_cols(expert_in, up_w)
    gate_sig = jax.nn.sigmoid(gate_pre)
    gate_act = gate_pre * gate_sig
    hidden = (gate_act * up_pre).astype(jnp.bfloat16)
    hidden_grad = contract_cols(expert_cot, down_w)
    gate_delta = (hidden_grad * up_pre * gate_sig * (1.0 + gate_pre * (1.0 - gate_sig))).astype(
        jnp.bfloat16
    )
    up_delta = (hidden_grad * gate_act).astype(jnp.bfloat16)
    partial_value = jnp.dot(gate_delta, gate_w, preferred_element_type=jnp.float32) + jnp.dot(
        up_delta, up_w, preferred_element_type=jnp.float32
    )
    stream_full, proj_full = combine(
        partial_value.astype(jnp.bfloat16), cotangent, pick, out_proj, experts
    )
    down_g = contract_rows(hidden, expert_cot).astype(jnp.bfloat16)
    gate_g = contract_rows(gate_delta, expert_in).astype(jnp.bfloat16)
    up_g = contract_rows(up_delta, expert_in).astype(jnp.bfloat16)
    proj_g, value_g, gating_g = module(
        stream_full,
        proj_full,
        mixed_all,
        conv_out,
        row_mean[:, None],
        row_rstd[:, None],
        ln_gain[None, :],
        taps,
        v_value,
        v_gate,
        experts,
    )
    stream = lax.dynamic_slice_in_dim(stream_full, lax.axis_index("tp") * width, width, 1)
    return (gate_g[None], up_g[None], down_g[None], proj_g, stream, value_g, gating_g)


def shards(*blocks):
    tokens, width = blocks[0].shape
    depth, channels = blocks[-1].shape
    experts = lax.axis_size("sp")
    square = lax.axis_size("tp") == 4 and experts % 2 == 0 and tokens == 128
    capacity = 4 * tokens // experts
    tiled = width % 128 == 0 and depth % 128 == 0 and channels % 128 == 0 and capacity % 16 == 0
    if square and tiled:
        return kernel_shards(*blocks)
    return plain_shards(*blocks)


def solution(mesh):
    return jax.shard_map(
        shards,
        mesh=mesh,
        in_specs=(
            P("sp", "tp"),
            P("sp", "tp"),
            P("sp", None),
            P("sp", None),
            P("sp", "tp", None),
            P("sp", "tp", None),
            P("sp", "tp", None),
            P("sp", "tp"),
            P("sp", "tp"),
            P("sp", "tp"),
            P("sp"),
            P("sp"),
            P("tp"),
            P(None, "tp"),
            P("sp", "tp"),
        ),
        out_specs=(
            P("sp", "tp", None),
            P("sp", "tp", None),
            P("sp", "tp", None),
            P("sp", "tp"),
            P("sp", "tp"),
            P("sp", "tp"),
            P("sp", "tp"),
        ),
        check_vma=False,
    )
```

```python
import functools

import jax
import jax.numpy as jnp
from jax import lax
from jax.experimental import pallas as pl
from jax.experimental.pallas import tpu as pltpu
from jax.sharding import PartitionSpec as P


def passed_along(value, axis, steps):
    count = lax.axis_size(axis)
    leading, last = (max(0, -steps), min(count, count - steps))
    return lax.ppermute(value, axis, [(source, source + steps) for source in range(leading, last)])


def route_targets(routes, experts, capacity):
    flat_routes = routes.reshape(-1)
    member = (flat_routes[:, None] == jnp.arange(experts, dtype=jnp.int32)[None, :]).astype(
        jnp.int32
    )
    earlier = jnp.cumsum(member, axis=0) - member
    slot_index = jnp.sum(earlier * member, axis=1)
    return flat_routes * capacity + slot_index


def contract_rows(left, right):
    return lax.dot_general(
        left, right, (((0,), (0,)), ((), ())), preferred_element_type=jnp.float32
    )


def contract_cols(left, right):
    return lax.dot_general(
        left, right, (((1,), (1,)), ((), ())), preferred_element_type=jnp.float32
    )


def plain_shards(
    moe_input,
    cotangent,
    routes,
    route_weight,
    w_gate,
    w_up,
    w_down,
    v_value,
    v_gate,
    conv_out,
    row_mean,
    row_rstd,
    ln_gain,
    taps,
    out_proj,
):
    experts = lax.axis_size("sp")
    tokens = routes.shape[0]
    capacity = 4 * tokens // experts
    total = experts * capacity
    buffer_row = route_targets(routes, experts, capacity)
    token_index = jnp.arange(2 * tokens, dtype=jnp.int32) // 2
    weights = route_weight.reshape(-1)
    width = moe_input.shape[1]
    picked = moe_input[token_index]
    weighted = (weights[:, None] * cotangent[token_index].astype(jnp.float32)).astype(jnp.bfloat16)
    rows_buf = jnp.zeros((total, width), jnp.bfloat16).at[buffer_row].set(picked)
    cotan_buf = jnp.zeros((total, width), jnp.bfloat16).at[buffer_row].set(weighted)
    rows_buf, cotan_buf = (
        rows_buf.reshape(experts, capacity, width),
        cotan_buf.reshape(experts, capacity, width),
    )
    part_rows, part_cotan = (
        lax.all_to_all(rows_buf, "sp", split_axis=0, concat_axis=0, tiled=True),
        lax.all_to_all(cotan_buf, "sp", split_axis=0, concat_axis=0, tiled=True),
    )
    arrived_rows, arrived_cotan = (
        lax.all_gather(part_rows, "tp", axis=2, tiled=True),
        lax.all_gather(part_cotan, "tp", axis=2, tiled=True),
    )
    width = arrived_rows.shape[2]
    expert_in = arrived_rows.reshape(total, width)
    expert_cot = arrived_cotan.reshape(total, width)
    gate_w = w_gate[0]
    up_w = w_up[0]
    down_w = w_down[0]
    gate_pre = contract_cols(expert_in, gate_w)
    up_pre = contract_cols(expert_in, up_w)
    gate_sig = jax.nn.sigmoid(gate_pre)
    gate_act = gate_pre * gate_sig
    hidden = (gate_act * up_pre).astype(jnp.bfloat16)
    down_g = contract_rows(hidden, expert_cot).astype(jnp.bfloat16)
    hidden_grad = contract_cols(expert_cot, down_w)
    gate_delta = (hidden_grad * up_pre * gate_sig * (1.0 + gate_pre * (1.0 - gate_sig))).astype(
        jnp.bfloat16
    )
    up_delta = (hidden_grad * gate_act).astype(jnp.bfloat16)
    gate_g = contract_rows(gate_delta, expert_in).astype(jnp.bfloat16)
    up_g = contract_rows(up_delta, expert_in).astype(jnp.bfloat16)
    partial_value = jnp.dot(gate_delta, gate_w, preferred_element_type=jnp.float32) + jnp.dot(
        up_delta, up_w, preferred_element_type=jnp.float32
    )
    row_share = lax.psum_scatter(
        partial_value.astype(jnp.bfloat16), "tp", scatter_dimension=1, tiled=True
    )
    slice_width = row_share.shape[1]
    returned = lax.all_to_all(
        row_share.reshape(experts, capacity, slice_width),
        "sp",
        split_axis=0,
        concat_axis=0,
        tiled=True,
    )
    mine = (
        returned.reshape(total, slice_width)[buffer_row]
        .astype(jnp.float32)
        .reshape(tokens, 2, slice_width)
    )
    stream = (cotangent.astype(jnp.float32) + (mine[:, 0] + mine[:, 1])).astype(jnp.bfloat16)
    full_stream = lax.all_gather(stream, "tp", axis=1, tiled=True)
    normed = (conv_out.astype(jnp.float32) - row_mean[:, None]) * row_rstd[:, None]
    scaled_norm = normed * ln_gain[None, :]
    norm_sig = jax.nn.sigmoid(scaled_norm)
    mixed = (scaled_norm * norm_sig).astype(jnp.bfloat16)
    columns = full_stream
    mixed_grad = jnp.dot(
        columns,
        lax.all_gather(out_proj, "sp", axis=0, tiled=True),
        preferred_element_type=jnp.float32,
    )
    columns = full_stream
    proj_g = lax.psum_scatter(
        contract_rows(columns, mixed).astype(jnp.bfloat16), "sp", scatter_dimension=0, tiled=True
    ).astype(jnp.float32)
    channels = out_proj.shape[1] * lax.axis_size("tp")
    norm_grad = mixed_grad * norm_sig * (1.0 + scaled_norm * (1.0 - norm_sig)) * ln_gain[None, :]
    first_sum, second_sum = lax.psum(
        (jnp.sum(norm_grad, axis=1), jnp.sum(norm_grad * normed, axis=1)), "tp"
    )
    first_mean = first_sum[:, None] / channels
    second_mean = second_sum[:, None] / channels
    conv_grad = row_rstd[:, None] * (norm_grad - first_mean - normed * second_mean)
    kernel = taps.shape[0]
    following = passed_along(conv_grad[: kernel - 1], "sp", -1)
    extended = jnp.concatenate([conv_grad, following], axis=0)
    tap_values = taps.astype(jnp.float32)
    unit_grad = jnp.zeros_like(conv_grad)
    for offset in range(kernel):
        lead = kernel - 1 - offset
        unit_grad = unit_grad + tap_values[offset][None, :] * extended[lead : lead + tokens]
    value_sig = jax.nn.sigmoid(v_gate.astype(jnp.float32))
    value_g = (unit_grad * value_sig).astype(jnp.bfloat16)
    gating_g = (unit_grad * v_value.astype(jnp.float32) * value_sig * (1.0 - value_sig)).astype(
        jnp.bfloat16
    )
    return (gate_g[None], up_g[None], down_g[None], proj_g, stream, value_g, gating_g)


VMEM = pl.BlockSpec(memory_space=pltpu.VMEM)


def remote(src, dst, send_sem, recv_sem, sp, tp):
    return pltpu.make_async_remote_copy(
        src_ref=src,
        dst_ref=dst,
        send_sem=send_sem,
        recv_sem=recv_sem,
        device_id={"sp": sp, "tp": tp},
        device_id_type=pl.DeviceIdType.MESH,
    )


def greet(peers):
    barrier = pltpu.get_barrier_semaphore()
    for sp, tp in peers:
        pl.semaphore_signal(
            barrier, inc=1, device_id={"sp": sp, "tp": tp}, device_id_type=pl.DeviceIdType.MESH
        )
    pl.semaphore_wait(barrier, len(peers))


def rows_of(ref, index, count):
    return ref.at[pl.ds(pl.multiple_of(index * count, count), count)]


class ChipGather:
    def __init__(self, own, everyone, sems, me, tp, count):
        self.own, self.everyone, self.me, self.tp, self.count = own, everyone, me, tp, count
        self.send, self.recv, self.relay, self.local = sems
        self.partner = me + 1 - 2 * (me % 2)
        self.ahead = [(me + 2 * e) % count for e in range(1, count // 2)]
        self.behind = [(me + count - 2 * e) % count for e in range(1, count // 2)]

    def block(self, index):
        return rows_of(self.everyone, index, self.own.shape[0])

    def first(self, target):
        return remote(
            self.own,
            self.block(self.me),
            self.send.at[target],
            self.recv.at[self.me],
            target,
            self.tp,
        )

    def onward(self, origin):
        return remote(
            self.block(origin),
            self.block(origin),
            self.relay.at[origin],
            self.recv.at[origin],
            self.partner,
            self.tp,
        )

    def start(self):
        pltpu.make_async_copy(self.own, self.block(self.me), self.local).start()
        for target in self.ahead + [self.partner]:
            self.first(target).start()

    def pass_on(self):
        for origin in self.behind:
            self.onward(origin).wait_recv()
            self.onward(origin).start()

    def finish(self):
        pltpu.make_async_copy(self.own, self.block(self.me), self.local).wait()
        for step in range(self.count // 2):
            origin = (self.partner + 2 * step) % self.count
            self.onward(origin).wait_recv()
        for target in self.ahead + [self.partner]:
            self.first(target).wait_send()
        for origin in self.behind:
            self.onward(origin).wait_send()


def gather_sems(count):
    return [
        pltpu.SemaphoreType.DMA((count,)),
        pltpu.SemaphoreType.DMA((count,)),
        pltpu.SemaphoreType.DMA((count,)),
        pltpu.SemaphoreType.DMA,
    ]


def dispatch_kernel(
    count, rows, cot, mixed, rows_out, cot_out, mixed_out, send, recv, local, *mixed_sems
):
    me, tp = lax.axis_index("sp"), lax.axis_index("tp")
    capacity, width = rows.shape[1:]
    across, down, corner = tp + 1 - 2 * (tp % 2), (tp + 2) % 4, 3 - tp
    others = [(me + d) % count for d in range(1, count)]
    greet([(other, tp) for other in others] + [(me, across), (me, down)])
    arrays = ((rows, rows_out), (cot, cot_out))

    def block(a, source, owner):
        return arrays[a][1].at[
            pl.ds(pl.multiple_of(source * capacity, capacity), capacity),
            pl.ds(pl.multiple_of(owner * width, 128), width),
        ]

    def own_copy(a):
        return pltpu.make_async_copy(arrays[a][0].at[me], block(a, me, tp), local.at[a])

    def out_copy(a, target):
        return remote(
            arrays[a][0].at[target],
            block(a, me, tp),
            send.at[a, target, 0],
            recv.at[a, me, tp],
            target,
            tp,
        )

    def side_copy(a, source, owner, target, lane):
        spot = block(a, source, owner)
        return remote(spot, spot, send.at[a, source, lane], recv.at[a, source, owner], me, target)

    for a in range(2):
        own_copy(a).start()
    for target in others:
        for a in range(2):
            out_copy(a, target).start()
    gather = ChipGather(mixed, mixed_out, mixed_sems, me, tp, count)
    gather.start()

    def relay_of(step):
        return (across, down) if step % 2 == 0 else (down, across)

    def relay(step):
        source = (me + count - step) % count
        owner, target = relay_of(step)
        for a in range(2):
            side_copy(a, source, owner, target, 3).wait_recv()
            side_copy(a, source, owner, target, 3).start()

    for step in range(count):
        source = (me + count - step) % count
        for a in range(2):
            if step == 0:
                own_copy(a).wait()
            else:
                side_copy(a, source, tp, across, 1).wait_recv()
            side_copy(a, source, tp, across, 1).start()
            side_copy(a, source, tp, down, 2).start()
        if step >= 1:
            relay(step - 1)
    relay(count - 1)
    gather.pass_on()
    for step in range(count):
        source = (me + count - step) % count
        owner, target = relay_of(step)
        for a in range(2):
            side_copy(a, source, target, across, 1).wait_recv()
            side_copy(a, source, corner, across, 1).wait_recv()
            side_copy(a, source, tp, across, 1).wait_send()
            side_copy(a, source, tp, down, 2).wait_send()
            side_copy(a, source, owner, target, 3).wait_send()
    for target in others:
        for a in range(2):
            out_copy(a, target).wait_send()
    gather.finish()


def dispatch(rows, cot, mixed, count):
    capacity, width = rows.shape[1:]
    full = jax.ShapeDtypeStruct((count * capacity, width * lax.axis_size("tp")), jnp.bfloat16)
    return pl.pallas_call(
        functools.partial(dispatch_kernel, count),
        out_shape=(
            full,
            full,
            jax.ShapeDtypeStruct((count * mixed.shape[0], mixed.shape[1]), mixed.dtype),
        ),
        in_specs=[VMEM] * 3,
        out_specs=(VMEM,) * 3,
        scratch_shapes=[
            pltpu.SemaphoreType.DMA((2, count, 4)),
            pltpu.SemaphoreType.DMA((2, count, 4)),
            pltpu.SemaphoreType.DMA((2,)),
        ]
        + gather_sems(count),
        compiler_params=pltpu.CompilerParams(
            collective_id=0, has_side_effects=True, vmem_limit_bytes=40 << 20
        ),
        name="dispatch",
        cost_estimate=pl.CostEstimate(
            flops=0, bytes_accessed=200 * rows.size * 2, transcendentals=0
        ),
    )(rows, cot, mixed)


def combine_kernel(
    count,
    partial_ref,
    cot,
    pick,
    proj,
    hidden,
    gate_delta,
    up_delta,
    expert_in,
    expert_cot,
    stream,
    proj_out,
    grads,
    landed,
    middle,
    reduced,
    back,
    send,
    recv,
    back_send,
    back_recv,
    wide_send,
    wide_recv,
    *proj_sems,
):
    me, tp = lax.axis_index("sp"), lax.axis_index("tp")
    capacity, width = reduced.shape[1:]
    units = hidden.shape[0]
    across, down, corner = tp + 1 - 2 * (tp % 2), (tp + 2) % 4, 3 - tp
    group = (across, down, corner)
    others = [(me + d) % count for d in range(1, count)]
    greet([(other, tp) for other in others] + [(me, other) for other in group])

    def share(source, owner):
        return partial_ref.at[
            pl.ds(pl.multiple_of(source * capacity, capacity), capacity),
            pl.ds(pl.multiple_of(owner * width, 128), width),
        ]

    order = others + [me]

    def sides(step):
        return (across, down) if step % 2 == 0 else (down, across)

    def share_copy(step, q):
        source, near = order[step], sides(step)[0]
        return remote(
            share(source, corner if q == 1 else near),
            landed.at[q, source],
            send.at[source, q],
            recv.at[source, q],
            me,
            near,
        )

    def middle_copy(step):
        source = order[step]
        return remote(
            middle.at[source],
            landed.at[2, source],
            send.at[source, 2],
            recv.at[source, 2],
            me,
            sides(step)[1],
        )

    def back_copy(target):
        return remote(
            reduced.at[target],
            rows_of(back, me, capacity),
            back_send.at[target],
            back_recv.at[me],
            target,
            tp,
        )

    def begin(step):
        for q in (1, 0):
            share_copy(step, q).start()

    def forward(step):
        source = order[step]
        share_copy(step, 1).wait_recv()
        own = share(source, sides(step)[1])[...].astype(jnp.float32)
        middle[source] = (own + landed[1, source].astype(jnp.float32)).astype(jnp.bfloat16)
        middle_copy(step).start()

    def settle(step):
        source = order[step]
        share_copy(step, 0).wait_recv()
        middle_copy(step).wait_recv()
        total = share(source, tp)[...].astype(jnp.float32)
        total = total + landed[0, source].astype(jnp.float32)
        total = (total + landed[2, source].astype(jnp.float32)).astype(jnp.bfloat16)
        if step < count - 1:
            reduced[source] = total
            back_copy(source).start()
        else:
            back[pl.ds(pl.multiple_of(me * capacity, capacity), capacity), :] = total

    pieces = 4 if units % 64 == 0 else 1
    tile = units // pieces
    spots = pieces * 4
    products = ((gate_delta, expert_in), (up_delta, expert_in), (hidden, expert_cot))

    def product(spot, carry):
        rows = pl.ds(pl.multiple_of(spot // 4 * tile, 16), tile)
        columns = pl.ds(pl.multiple_of(spot % 4 * width, 128), width)
        for a, (left, right) in enumerate(products):
            value = jnp.dot(
                left[rows, :], right[:, columns], preferred_element_type=jnp.float32
            )
            grads[a, rows, columns] = value.astype(jnp.bfloat16)
        return carry

    window = min(3, count)
    for step in range(window):
        begin(step)
    gather = ChipGather(proj, proj_out, proj_sems, me, tp, count)
    gather.start()
    for step in range(count):
        lax.fori_loop(spots * step // count, spots * (step + 1) // count, product, 0)
        if step + window < count:
            begin(step + window)
        forward(step)
        if step >= 1:
            settle(step - 1)
    settle(count - 1)
    gather.pass_on()
    for other in others:
        remote(
            reduced.at[other],
            rows_of(back, other, capacity),
            back_send.at[other],
            back_recv.at[other],
            other,
            tp,
        ).wait_recv()
    mine = jnp.dot(pick[...], back[...], preferred_element_type=jnp.float32)
    columns = pl.ds(pl.multiple_of(tp * width, 128), width)
    stream[:, columns] = (cot[...].astype(jnp.float32) + mine).astype(jnp.bfloat16)

    def wide_copy(q):
        spot = stream.at[:, columns]
        return remote(spot, spot, wide_send.at[q], wide_recv.at[q], me, group[q])

    for q in range(3):
        wide_copy(q).start()
    for q in range(3):
        wide_copy(q).wait()
    for step in range(count):
        share_copy(step, 0).wait_send()
        share_copy(step, 1).wait_send()
        middle_copy(step).wait_send()
    for other in others:
        back_copy(other).wait_send()
    gather.finish()


def combine(partial_value, cot, pick, proj, hidden, gate_delta, up_delta, rows, rows_cot, count):
    tokens, width = cot.shape
    capacity = partial_value.shape[0] // count
    return pl.pallas_call(
        functools.partial(combine_kernel, count),
        out_shape=(
            jax.ShapeDtypeStruct((tokens, partial_value.shape[1]), jnp.bfloat16),
            jax.ShapeDtypeStruct((count * proj.shape[0], proj.shape[1]), jnp.bfloat16),
            jax.ShapeDtypeStruct((3, hidden.shape[0], partial_value.shape[1]), jnp.bfloat16),
        ),
        in_specs=[VMEM] * 9,
        out_specs=(VMEM,) * 3,
        scratch_shapes=[
            pltpu.VMEM((3, count, capacity, width), jnp.bfloat16),
            pltpu.VMEM((count, capacity, width), jnp.bfloat16),
            pltpu.VMEM((count, capacity, width), jnp.bfloat16),
            pltpu.VMEM((count * capacity, width), jnp.bfloat16),
            pltpu.SemaphoreType.DMA((count, 3)),
            pltpu.SemaphoreType.DMA((count, 3)),
            pltpu.SemaphoreType.DMA((count,)),
            pltpu.SemaphoreType.DMA((count,)),
            pltpu.SemaphoreType.DMA((3,)),
            pltpu.SemaphoreType.DMA((3,)),
        ]
        + gather_sems(count),
        compiler_params=pltpu.CompilerParams(
            collective_id=1, has_side_effects=True, vmem_limit_bytes=40 << 20
        ),
        name="combine",
        cost_estimate=pl.CostEstimate(
            flops=6 * hidden.size * partial_value.shape[1],
            bytes_accessed=50 * partial_value.size * 2,
            transcendentals=0,
        ),
    )(partial_value, cot, pick, proj, hidden, gate_delta, up_delta, rows, rows_cot)


def module_kernel(
    count,
    stream,
    proj,
    mixed,
    conv_out,
    row_mean,
    row_rstd,
    gain,
    taps,
    v_value,
    v_gate,
    proj_grad,
    value_grad,
    gating_grad,
    columns,
    sums,
    arrived,
    extended,
    send,
    recv,
    local,
    sum_send,
    sum_recv,
    edge_send,
    edge_recv,
):
    me, tp = lax.axis_index("sp"), lax.axis_index("tp")
    tokens, channels = conv_out.shape
    depth = stream.shape[1] // count
    halo = extended.shape[0] - tokens
    group = (tp + 1 - 2 * (tp % 2), (tp + 2) % 4, 3 - tp)
    others = [(me + d) % count for d in range(1, count)]
    greet([(other, tp) for other in others] + [(me, other) for other in group])

    def strip(index):
        return stream.at[:, pl.ds(pl.multiple_of(index * depth, 128), depth)]

    def strip_copy(target):
        return remote(
            strip(target),
            rows_of(columns, me, tokens),
            send.at[target],
            recv.at[me],
            target,
            tp,
        )

    own = pltpu.make_async_copy(strip(me), rows_of(columns, me, tokens), local)
    own.start()
    for other in others:
        strip_copy(other).start()
    mixed_grad = jnp.dot(stream[...], proj[...], preferred_element_type=jnp.float32)
    rstd = jnp.broadcast_to(row_rstd[...], (tokens, tokens)).T[:, 0:1]
    mean = jnp.broadcast_to(row_mean[...], (tokens, tokens)).T[:, 0:1]
    normed = (conv_out[...].astype(jnp.float32) - mean) * rstd
    scaled = normed * gain[...]
    sig = jax.nn.sigmoid(scaled)
    norm_grad = mixed_grad * sig * (1.0 + scaled * (1.0 - sig)) * gain[...]
    first = jnp.sum(norm_grad, axis=1, keepdims=True)
    second = jnp.sum(norm_grad * normed, axis=1, keepdims=True)
    lanes = lax.broadcasted_iota(jnp.int32, (tokens, 128), 1)
    pair = jnp.where(lanes % 2 == 0, first, second)
    sums[...] = pair.T[:8]

    def sum_copy(q):
        return remote(sums, arrived.at[q], sum_send.at[q], sum_recv.at[q], me, group[q])

    for q in range(3):
        sum_copy(q).start()
    value_sig = jax.nn.sigmoid(v_gate[...].astype(jnp.float32))
    gating_scale = v_value[...].astype(jnp.float32) * value_sig * (1.0 - value_sig)
    for q in range(3):
        sum_copy(q).wait()
    total = sums[...] + arrived[0] + arrived[1] + arrived[2]
    total = total * (1.0 / (channels * 4))
    means = jnp.concatenate([total] * 16, axis=0).T
    conv_grad = rstd * (norm_grad - means[:, 0:1] - normed * means[:, 1:2])
    extended[:tokens] = conv_grad
    edge = remote(
        extended.at[pl.ds(0, halo)],
        extended.at[pl.ds(tokens, halo)],
        edge_send,
        edge_recv,
        (me + count - 1) % count,
        tp,
    )

    @pl.when(me > 0)
    def _():
        edge.start()

    @pl.when(me == count - 1)
    def _():
        extended[tokens:] = jnp.zeros((halo, channels), jnp.float32)

    @pl.when(me < count - 1)
    def _():
        edge.wait_recv()

    kernel = taps.shape[0]
    unit_grad = jnp.zeros((tokens, channels), jnp.float32)
    for offset in range(kernel):
        lead = kernel - 1 - offset
        tap = taps[offset : offset + 1, :].astype(jnp.float32)
        unit_grad = unit_grad + tap * extended[lead : lead + tokens, :]
    value_grad[...] = (unit_grad * value_sig).astype(jnp.bfloat16)
    gating_grad[...] = (unit_grad * gating_scale).astype(jnp.bfloat16)
    own.wait()
    for other in others:
        remote(
            strip(other),
            rows_of(columns, other, tokens),
            send.at[other],
            recv.at[other],
            other,
            tp,
        ).wait_recv()
    proj_grad[...] = contract_rows(columns[...], mixed[...])
    for other in others:
        strip_copy(other).wait_send()

    @pl.when(me > 0)
    def _():
        edge.wait_send()


def module(stream, proj, mixed, conv_out, row_mean, row_rstd, gain, taps, v_value, v_gate, count):
    tokens, channels = conv_out.shape
    depth = stream.shape[1] // count
    halo = -(-(taps.shape[0] - 1) // 8) * 8
    return pl.pallas_call(
        functools.partial(module_kernel, count),
        out_shape=(
            jax.ShapeDtypeStruct((depth, channels), jnp.float32),
            jax.ShapeDtypeStruct((tokens, channels), jnp.bfloat16),
            jax.ShapeDtypeStruct((tokens, channels), jnp.bfloat16),
        ),
        in_specs=[VMEM] * 10,
        out_specs=(VMEM,) * 3,
        scratch_shapes=[
            pltpu.VMEM((count * tokens, depth), jnp.bfloat16),
            pltpu.VMEM((8, tokens), jnp.float32),
            pltpu.VMEM((3, 8, tokens), jnp.float32),
            pltpu.VMEM((tokens + halo, channels), jnp.float32),
            pltpu.SemaphoreType.DMA((count,)),
            pltpu.SemaphoreType.DMA((count,)),
            pltpu.SemaphoreType.DMA,
            pltpu.SemaphoreType.DMA((3,)),
            pltpu.SemaphoreType.DMA((3,)),
            pltpu.SemaphoreType.DMA,
            pltpu.SemaphoreType.DMA,
        ],
        compiler_params=pltpu.CompilerParams(
            collective_id=2, has_side_effects=True, vmem_limit_bytes=40 << 20
        ),
        name="module",
    )(stream, proj, mixed, conv_out, row_mean, row_rstd, gain, taps, v_value, v_gate)


def kernel_shards(
    moe_input,
    cotangent,
    routes,
    route_weight,
    w_gate,
    w_up,
    w_down,
    v_value,
    v_gate,
    conv_out,
    row_mean,
    row_rstd,
    ln_gain,
    taps,
    out_proj,
):
    experts = lax.axis_size("sp")
    tokens, width = moe_input.shape
    capacity = 4 * tokens // experts
    total = experts * capacity
    flat_routes = routes.reshape(-1)
    member = (flat_routes[:, None] == jnp.arange(experts, dtype=jnp.int32)[None, :]).astype(
        jnp.bfloat16
    )
    index = jnp.arange(2 * tokens, dtype=jnp.int32)
    before = (index[None, :] < index[:, None]).astype(jnp.bfloat16)
    earlier = jnp.dot(before, member, preferred_element_type=jnp.float32)
    slot_index = jnp.sum(earlier * member.astype(jnp.float32), axis=1).astype(jnp.int32)
    buffer_row = (flat_routes * capacity + slot_index).reshape(tokens, 2)
    places = jnp.arange(total, dtype=jnp.int32)
    place0 = (buffer_row[:, 0][:, None] == places[None, :]).astype(jnp.bfloat16)
    place1 = (buffer_row[:, 1][:, None] == places[None, :]).astype(jnp.bfloat16)
    pick = place0 + place1
    cot32 = cotangent.astype(jnp.float32)
    weighted = jnp.concatenate(
        [
            (route_weight[:, 0:1] * cot32).astype(jnp.bfloat16),
            (route_weight[:, 1:2] * cot32).astype(jnp.bfloat16),
        ],
        axis=0,
    )
    rows_buf = contract_rows(pick, moe_input).astype(jnp.bfloat16)
    cot_buf = contract_rows(jnp.concatenate([place0, place1], axis=0), weighted).astype(
        jnp.bfloat16
    )
    normed = (conv_out.astype(jnp.float32) - row_mean[:, None]) * row_rstd[:, None]
    scaled_norm = normed * ln_gain[None, :]
    mixed = (scaled_norm * jax.nn.sigmoid(scaled_norm)).astype(jnp.bfloat16)
    expert_in, expert_cot, mixed_all = dispatch(
        rows_buf.reshape(experts, capacity, width),
        cot_buf.reshape(experts, capacity, width),
        mixed,
        experts,
    )
    gate_w = w_gate[0]
    up_w = w_up[0]
    down_w = w_down[0]
    gate_pre = contract_cols(gate_w, expert_in)
    up_pre = contract_cols(up_w, expert_in)
    gate_sig = jax.nn.sigmoid(gate_pre)
    gate_act = gate_pre * gate_sig
    hidden = (gate_act * up_pre).astype(jnp.bfloat16)
    hidden_grad = contract_cols(down_w, expert_cot)
    gate_delta = (hidden_grad * up_pre * gate_sig * (1.0 + gate_pre * (1.0 - gate_sig))).astype(
        jnp.bfloat16
    )
    up_delta = (hidden_grad * gate_act).astype(jnp.bfloat16)
    partial_value = contract_rows(gate_delta, gate_w) + contract_rows(up_delta, up_w)
    stream_full, proj_full, grads = combine(
        partial_value.astype(jnp.bfloat16),
        cotangent,
        pick,
        out_proj,
        hidden,
        gate_delta,
        up_delta,
        expert_in,
        expert_cot,
        experts,
    )
    proj_g, value_g, gating_g = module(
        stream_full,
        proj_full,
        mixed_all,
        conv_out,
        row_mean[None, :],
        row_rstd[None, :],
        ln_gain[None, :],
        taps,
        v_value,
        v_gate,
        experts,
    )
    stream = lax.dynamic_slice_in_dim(stream_full, lax.axis_index("tp") * width, width, 1)
    return (grads[0:1], grads[1:2], grads[2:3], proj_g, stream, value_g, gating_g)


def shards(*blocks):
    tokens, width = blocks[0].shape
    depth, channels = blocks[-1].shape
    experts = lax.axis_size("sp")
    square = lax.axis_size("tp") == 4 and experts % 2 == 0 and tokens == 128
    capacity = 4 * tokens // experts
    tiled = width % 128 == 0 and depth % 128 == 0 and channels % 128 == 0 and capacity % 16 == 0
    if square and tiled:
        return kernel_shards(*blocks)
    return plain_shards(*blocks)


def solution(mesh):
    return jax.shard_map(
        shards,
        mesh=mesh,
        in_specs=(
            P("sp", "tp"),
            P("sp", "tp"),
            P("sp", None),
            P("sp", None),
            P("sp", "tp", None),
            P("sp", "tp", None),
            P("sp", "tp", None),
            P("sp", "tp"),
            P("sp", "tp"),
            P("sp", "tp"),
            P("sp"),
            P("sp"),
            P("tp"),
            P(None, "tp"),
            P("sp", "tp"),
        ),
        out_specs=(
            P("sp", "tp", None),
            P("sp", "tp", None),
            P("sp", "tp", None),
            P("sp", "tp"),
            P("sp", "tp"),
            P("sp", "tp"),
            P("sp", "tp"),
        ),
        check_vma=False,
    )
```
